32 devices in a mesh: grp: 2 (over y), ep: 4 (over z), tp: 4 (over x, core).
Axes of the slice: x: 2, y: 2, z: 4, core: 2. Of those that a mesh axis runs over, the one named last changes fastest.
Arguments:
- query: bfloat16 [8192, 1024], P(('grp', 'ep'), 'tp'), parts along dimension 0, may hold values from -6 to 6
- forget_gate_logits: bfloat16 [8192, 1024], P(('grp', 'ep'), 'tp'), parts along dimension 0, may hold values from -8 to 8
- value: bfloat16 [8192, 1024], P(('grp', 'ep'), 'tp'), parts along dimension 0, may hold values from -6 to 6
- forget_lower_margin: float32 [2, 1024], P(None, 'tp'), may hold values from -30 to -2
- position_log_decay: float32 [8, 8192], P('tp', ('grp', 'ep')), parts along dimension 1, may hold values from -1.5 to 0
- head_norm_gain: float32 [128], replicated, may hold values from 0.1 to 1.9
- mixer_output_weight: bfloat16 [1024, 2048], P('tp'), may hold values from -0.1875 to 0.1875
- second_batch_tokens: bfloat16 [4096, 2048], P(('grp', 'ep', 'tp')), parts along dimension 0, may hold values from -60 to 60
- expert_norm_gain: float32 [2048], replicated, may hold values from 0.1 to 1.9
- routes: int32 [4096, 2], P(('grp', 'ep', 'tp')), parts along dimension 0, may hold values from 0 to 3, all different within a row; in each aligned block of 128 rows (0 to 127, 128 to 255, ...) at most 96 rows name the same one
- chosen_expert_weight: float32 [4096, 2], P(('grp', 'ep', 'tp')), parts along dimension 0, may hold values from 0.2 to 1
- gate_weight: bfloat16 [4, 2048, 2048], P('ep', None, 'tp'), may hold values from -0.3125 to 0.3125
- up_weight: bfloat16 [4, 2048, 2048], P('ep', None, 'tp'), may hold values from -0.3125 to 0.3125
- down_weight: bfloat16 [4, 2048, 2048], P('ep', 'tp'), may hold values from -0.02734375 to 0.02734375
Outputs:
- first_mixer_output: bfloat16 [8192, 2048], P(('grp', 'ep', 'tp')), parts along dimension 0
- moe_out: bfloat16 [4096, 2048], P(('grp', 'ep', 'tp')), parts along dimension 0
The draws below stay inside these ranges and needn't reach their ends.
There are 2 independent parts, one for each index of `grp`. The reference program is written for one: setup_inputs(seed, part) draws one part's arguments, and reference() takes and returns one part's arrays. A program takes and returns all parts, laid end to end along the dimension named above; an argument that names none is the same for every part. Nothing has to cross between parts.
Inputs may be any that keep to these rules, and one draw needn't show every extreme that they name: `routes`: each row names 2 different experts. Among the rows of one device no expert is named by more than 96 rows, and in every draw some expert is named by exactly 96 rows of some device.
All inputs are finite; a program needn't handle non-finite values.
Results may differ from the reference program's by a relative error of at most 0.015.
Values may be sent and summed in bfloat16 or wider, within the bound.
A program may use at most 128 MiB of HBM per device.

```python
import math
import jax
import jax.numpy as jnp
import numpy as np
from jax import lax

D = 2048
RECURRENT_HEADS = 8
HEAD_CHANNELS = 128
FF = 2048
TOPK = 2
BLK = 128
ROWS = 1024
TOK_DEV = 128
SEQUENCE_TOKENS = 4096
MOE_TOKENS = 2048
EXPERTS = 4
CAP = 96
HEAD_GROUP = 2
FF_GROUP = 512
N_EP = 4
N_TP = 4


def draw_forget_lower_margin(key, part):
    key = jax.random.fold_in(key, 101)
    pick_key, fast_key, slow_key = jax.random.split(key, 3)
    share = 0.5
    slow_heads = jax.random.uniform(pick_key, (2, RECURRENT_HEADS, 1)) < share
    fast_gap = jnp.log(jax.random.uniform(fast_key, (2, RECURRENT_HEADS, HEAD_CHANNELS), minval=0.02, maxval=0.06))
    slow_gap = jax.random.uniform(slow_key, (2, RECURRENT_HEADS, HEAD_CHANNELS), minval=jnp.log(0.1), maxval=jnp.log(0.4)) - jnp.log(float(SEQUENCE_TOKENS))
    chosen = jnp.where(slow_heads, slow_gap, fast_gap)
    return chosen.reshape(2, RECURRENT_HEADS * HEAD_CHANNELS).astype(jnp.float32)


def draw_position_log_decay(key, part):
    key = jax.random.fold_in(key, 202)
    rate_key, place_key, size_key = jax.random.split(key, 3)
    blocks = SEQUENCE_TOKENS // ROWS
    rates = jnp.exp(jax.random.uniform(rate_key, (RECURRENT_HEADS, blocks, 1), minval=jnp.log(0.15), maxval=jnp.log(0.6)))
    steady = jnp.broadcast_to(rates / SEQUENCE_TOKENS, (RECURRENT_HEADS, blocks, ROWS)).reshape(RECURRENT_HEADS, SEQUENCE_TOKENS)
    places = jax.random.randint(place_key, (RECURRENT_HEADS, 2), 0, SEQUENCE_TOKENS)
    sizes = jax.random.uniform(size_key, (RECURRENT_HEADS, 2), minval=0.22, maxval=0.69)
    positions = jnp.arange(SEQUENCE_TOKENS, dtype=jnp.int32)
    hits = jnp.sum(jnp.where(positions[None, None, :] == places[:, :, None], sizes[:, :, None], 0.0), axis=1)
    return (-steady - hits).astype(jnp.float32)


def draw_second_batch_tokens(key, part):
    key = jax.random.fold_in(key, 303)
    base_key, row_key, column_key = jax.random.split(key, 3)
    base = jnp.clip(jax.random.normal(base_key, (MOE_TOKENS, D)), -5.0, 5.0)
    row_scale = jnp.exp(jax.random.uniform(row_key, (MOE_TOKENS, 1), minval=jnp.log(0.3), maxval=jnp.log(3.0)))
    column_scale = jnp.exp(jax.random.uniform(column_key, (1, D), minval=jnp.log(0.4), maxval=jnp.log(4.0)))
    return (base * row_scale * column_scale).astype(jnp.bfloat16)


def level_of(own_key, dims, pieces, smallest, largest):
    factor_of, own = 1.0, jax.random.fold_in(own_key, 6)
    for axis_at, blocks in pieces:
        steps = jnp.exp(jax.random.uniform(jax.random.fold_in(own, axis_at), (blocks,), jnp.float32, smallest / len(pieces), largest / len(pieces)))
        factor_of = factor_of * jnp.repeat(steps, dims[axis_at] // blocks).reshape([-1 if axis == axis_at else 1 for axis in range(len(dims))])
    return factor_of


def routed_block(stream_key, own, number, rows, number_of, top, reach, skew):
    ranking = jax.random.permutation(stream_key, number_of)
    heavy_load, ordinary = load_shares(number_of, rows * top, reach, skew, True), load_shares(number_of, rows * top, reach, skew, False)
    places = jnp.arange(number_of)

    def named(tallies, turn):
        used = int((tallies > 0).sum())
        fixed = max(1, used // 4)
        shifted = fixed + (places - fixed + turn * (used - fixed)) % max(1, number_of - fixed)
        return jnp.zeros((number_of,), jnp.int32).at[ranking[jnp.where(places < fixed, places, shifted)]].set(jnp.asarray(tallies, jnp.int32))

    tallies = jnp.where(number % 4 == 0, named(heavy_load, number // 4), named(ordinary, number - number // 4 - 1))
    mixed = jax.random.permutation(jax.random.fold_in(own, 3), number_of)
    giver, sink = mixed[0:number_of // 2 * 2:2], mixed[1:number_of // 2 * 2:2]
    margin = jnp.minimum(tallies[giver] - 1, reach - tallies[sink]) // 2
    margin = jnp.where((giver == ranking[0]) | (sink == ranking[0]) | (tallies[sink] == 0), 0, jnp.maximum(margin, 0))
    shifted = jax.random.randint(jax.random.fold_in(own, 4), (number_of // 2,), 0, 1 << 20) % (margin + 1)
    tallies = tallies.at[giver].add(-shifted).at[sink].add(shifted)
    members = jnp.searchsorted(jnp.cumsum(tallies), jnp.arange(rows * top), side="right").astype(jnp.int32)
    grid = members.reshape(top, rows).T
    grid = grid[jax.random.permutation(jax.random.fold_in(own, 1), rows)]
    turn = jax.random.randint(jax.random.fold_in(own, 2), (rows, 1), 0, top)
    return jnp.take_along_axis(grid, (jnp.arange(top)[None, :] + turn) % top, axis=1)


def load_shares(count, total, limit, slope, full):
    loads = [(1 << 20) // math.isqrt(grade ** slope) + 1 for grade in range(1, count + 1)]
    largest = limit if full else min(limit, max(-(-total // count), total * loads[0] // sum(loads)))
    least = 1 if total - largest >= count - 1 else 0
    given, surplus = [largest] + [least] * (count - 1), total - largest - least * (count - 1)
    while surplus > 0:
        free = [i for i in range(1, count) if given[i] < largest] or [i for i in range(1, count) if given[i] < limit]
        whole, remaining = sum([loads[i] for i in free]), surplus
        for i in free:
            more = min(limit - given[i], max(1, remaining * loads[i] // whole), surplus)
            given[i] = given[i] + more
            surplus = surplus - more
    return np.array(given)


def noise(stream_key, dims, spread, most, cuts=(), kind=jnp.bfloat16):
    loudness = level_of(stream_key, dims, cuts, -0.22, 0.18) if cuts else 1.0
    values = jax.random.normal(stream_key, dims, jnp.float32) * spread * loudness
    return jnp.minimum(jnp.maximum(values, -most), most).astype(kind)


def setup_inputs(seed: int = 0, part: int = 0) -> dict:
    seeds = jax.random.split(jax.random.key(seed), 15)
    own_keys = jax.random.split(jax.random.fold_in(seeds[14], part), 15)
    query = noise(own_keys[0], (SEQUENCE_TOKENS, RECURRENT_HEADS * HEAD_CHANNELS), 1.0, 6.0, ((0, 4), (1, 4)))
    forget_gate_logits = noise(own_keys[1], (SEQUENCE_TOKENS, RECURRENT_HEADS * HEAD_CHANNELS), 1.5, 8.0, ((0, 4), (1, 4)))
    value = noise(own_keys[2], (SEQUENCE_TOKENS, RECURRENT_HEADS * HEAD_CHANNELS), 1.0, 6.0, ((0, 4), (1, 4)))
    forget_lower_margin = draw_forget_lower_margin(jax.random.fold_in(seeds[14], 71), part)
    position_log_decay = draw_position_log_decay(jax.random.fold_in(jax.random.fold_in(seeds[14], part), 71), part)
    head_norm_gain = jnp.clip(1.0 + 0.18 * jax.random.normal(seeds[5], (HEAD_CHANNELS,), jnp.float32), 0.1, 1.9)
    mixer_output_weight = noise(seeds[6], (RECURRENT_HEADS * HEAD_CHANNELS, D), (RECURRENT_HEADS * HEAD_CHANNELS) ** -0.5, 0.1875, ((0, 4),))
    second_batch_tokens = draw_second_batch_tokens(jax.random.fold_in(jax.random.fold_in(seeds[14], part), 71), part)
    expert_norm_gain = jnp.clip(1.0 + 0.18 * jax.random.normal(seeds[8], (D,), jnp.float32), 0.1, 1.9)
    routes_keys = jax.random.split(jax.random.fold_in(own_keys[9], 1), MOE_TOKENS // TOK_DEV)
    routes_turns = jax.random.permutation(jax.random.fold_in(own_keys[9], 3), MOE_TOKENS // TOK_DEV)
    routes = jax.vmap(lambda own, number: routed_block(jax.random.fold_in(own_keys[9], 2), own, number, TOK_DEV, EXPERTS, TOPK, CAP, 2))(routes_keys, routes_turns).reshape((MOE_TOKENS, TOPK))
    chosen_expert_weight = jnp.clip(0.2 + 0.8 * jax.random.uniform(own_keys[10], (MOE_TOKENS, TOPK), jnp.float32) ** level_of(own_keys[10], (MOE_TOKENS, TOPK), ((0, 16),), -0.2, 0.2), 0.2, 1.0)
    gate_weight = noise(seeds[11], (EXPERTS, D, FF), (D // 6) ** -0.5, 0.3125, ((0, 4), (2, 4)))
    up_weight = noise(seeds[12], (EXPERTS, D, FF), (D // 6) ** -0.5, 0.3125, ((0, 4), (2, 4)))
    down_weight = noise(seeds[13], (EXPERTS, FF, D), (25 * FF) ** -0.5, 0.02734375, ((0, 4), (1, 4)))
    return {"query": query, "forget_gate_logits": forget_gate_logits, "value": value, "forget_lower_margin": forget_lower_margin, "position_log_decay": position_log_decay, "head_norm_gain": head_norm_gain, "mixer_output_weight": mixer_output_weight, "second_batch_tokens": second_batch_tokens, "expert_norm_gain": expert_norm_gain, "routes": routes, "chosen_expert_weight": chosen_expert_weight, "gate_weight": gate_weight, "up_weight": up_weight, "down_weight": down_weight}


NORM_EPS = 1e-06
CLAMP_LIMIT = 7.0
SIGMOID_SCALE = 1.702
PRECISE = lax.Precision.HIGHEST

def clamped_unit(gate_pre, up_pre):
    gate_pre = jnp.minimum(gate_pre, CLAMP_LIMIT)
    up_pre = jnp.clip(up_pre, -CLAMP_LIMIT, CLAMP_LIMIT)
    return (up_pre + 1.0) * gate_pre * jax.nn.sigmoid(SIGMOID_SCALE * gate_pre)

def block_recurrence(queries, ending_state, values, forget_log_rates):
    sequence_length, number_of_heads, channels = queries.shape
    nblocks = sequence_length // BLK

    def to_blocks(array):
        return array.reshape(nblocks, BLK, number_of_heads, array.shape[-1])
    query_blocks = to_blocks(queries)
    key_blocks = to_blocks(ending_state)
    value_blocks = to_blocks(values)
    cumul = jnp.cumsum(to_blocks(forget_log_rates), axis=1)
    block_last = cumul[:, -1]
    query_in = query_blocks * jnp.exp(cumul)
    key_in = key_blocks * jnp.exp(-cumul)
    key_state = key_blocks * jnp.exp(block_last[:, None] - cumul)
    lower = jnp.tril(jnp.ones((BLK, BLK), jnp.float32))
    scores = jnp.einsum('nchd,nshd->nhcs', query_in, key_in, precision=PRECISE) * lower
    inner = jnp.einsum('nhcs,nshv->nchv', scores, value_blocks, precision=PRECISE)
    increments = jnp.einsum('nshd,nshv->nhdv', key_state, value_blocks, precision=PRECISE)

    def advance(state, inputs):
        decay, increment = inputs
        return (state * decay[..., None] + increment, state)
    initial = jnp.zeros((number_of_heads, channels, values.shape[-1]), jnp.float32)
    final_state, before = lax.scan(advance, initial, (jnp.exp(block_last), increments))
    outer = jnp.einsum('nchd,nhdv->nchv', query_in, before, precision=PRECISE)
    return (inner + outer).reshape(sequence_length, number_of_heads, values.shape[-1])

def token_mixer(query, forget_gate_logits, value, forget_lower_margin, position_log_decay, head_norm_gain, mixer_output_weight):
    queries = jax.nn.silu(query.astype(jnp.float32)).reshape(SEQUENCE_TOKENS, RECURRENT_HEADS, HEAD_CHANNELS) * HEAD_CHANNELS ** (-0.5)
    values = value.astype(jnp.float32).reshape(SEQUENCE_TOKENS, RECURRENT_HEADS, HEAD_CHANNELS)
    shutting = jax.nn.sigmoid(-forget_gate_logits.astype(jnp.float32))
    decay_spikes = jnp.transpose(position_log_decay)[:, :, None]
    mix = jnp.zeros((SEQUENCE_TOKENS, RECURRENT_HEADS, HEAD_CHANNELS), jnp.float32)
    for direction in range(2):
        ending_state = jnp.exp(forget_lower_margin[direction])[None, :] * shutting
        forget_log_rates = jnp.log1p(-ending_state).reshape(SEQUENCE_TOKENS, RECURRENT_HEADS, HEAD_CHANNELS) + decay_spikes
        ending_state = ending_state.reshape(SEQUENCE_TOKENS, RECURRENT_HEADS, HEAD_CHANNELS)
        if direction == 0:
            mix = mix + block_recurrence(queries, ending_state, values, forget_log_rates)
        else:
            turned = block_recurrence(jnp.flip(queries, 0), jnp.flip(ending_state, 0), jnp.flip(values, 0), jnp.flip(forget_log_rates, 0))
            mix = mix + jnp.flip(turned, 0)
    scaled = mix * lax.rsqrt(lax.optimization_barrier(jnp.mean(mix * mix, axis=-1, keepdims=True)) + NORM_EPS) * head_norm_gain
    head_outputs = scaled.reshape(SEQUENCE_TOKENS, RECURRENT_HEADS * HEAD_CHANNELS).astype(jnp.bfloat16)
    group_width = HEAD_GROUP * HEAD_CHANNELS
    summed = jnp.zeros((SEQUENCE_TOKENS, D), jnp.float32)
    for group in range(N_TP):
        part_sum = jnp.dot(head_outputs[:, group * group_width:(group + 1) * group_width], mixer_output_weight[group * group_width:(group + 1) * group_width], preferred_element_type=jnp.float32).astype(jnp.bfloat16)
        summed = summed + part_sum.astype(jnp.float32)
    return summed.astype(jnp.bfloat16)

def experts(second_batch_tokens, expert_norm_gain, routes, chosen_expert_weight, gate_weight, up_weight, down_weight):
    tokens_f = second_batch_tokens.astype(jnp.float32)
    normed = (tokens_f * lax.rsqrt(lax.optimization_barrier(jnp.mean(tokens_f * tokens_f, axis=-1, keepdims=True)) + NORM_EPS) * expert_norm_gain).astype(jnp.bfloat16)
    count = normed.shape[0]
    padded = jnp.concatenate([normed, jnp.zeros((1, D), jnp.bfloat16)], axis=0)
    flat_routes = routes.reshape(-1)
    scales_all = jnp.concatenate([chosen_expert_weight.reshape(-1), jnp.zeros((1,), jnp.float32)])
    most_rows = CAP * N_EP * N_TP

    def one_expert(running, expert):
        positions, = jnp.nonzero(flat_routes == expert, size=most_rows, fill_value=count * TOPK)
        positions = positions.astype(jnp.int32)
        owners = positions // TOPK
        picked_rows = padded[owners]
        scales = scales_all[positions]
        gate_pre = jnp.dot(picked_rows, gate_weight[expert], preferred_element_type=jnp.float32)
        up_pre = jnp.dot(picked_rows, up_weight[expert], preferred_element_type=jnp.float32)
        hidden = clamped_unit(gate_pre, up_pre).astype(jnp.bfloat16)
        result = jnp.zeros((most_rows, D), jnp.float32)
        for group in range(N_TP):
            part_sum = jnp.dot(hidden[:, group * FF_GROUP:(group + 1) * FF_GROUP], down_weight[expert, group * FF_GROUP:(group + 1) * FF_GROUP], preferred_element_type=jnp.float32).astype(jnp.bfloat16)
            result = result + part_sum.astype(jnp.float32)
        rounded = lax.optimization_barrier(result.astype(jnp.bfloat16)).astype(jnp.float32)
        running = running.at[owners].add(scales[:, None] * rounded)
        return (running, None)
    start_sum = jnp.zeros((count + 1, D), jnp.float32)
    total_sum, _ = lax.scan(one_expert, start_sum, jnp.arange(EXPERTS, dtype=jnp.int32))
    return total_sum[:count].astype(jnp.bfloat16)

def reference(query, forget_gate_logits, value, forget_lower_margin, position_log_decay, head_norm_gain, mixer_output_weight, second_batch_tokens, expert_norm_gain, routes, chosen_expert_weight, gate_weight, up_weight, down_weight):
    first_mixer_output = token_mixer(query, forget_gate_logits, value, forget_lower_margin, position_log_decay, head_norm_gain, mixer_output_weight)
    moe_out = experts(second_batch_tokens, expert_norm_gain, routes, chosen_expert_weight, gate_weight, up_weight, down_weight)
    return (first_mixer_output, moe_out)
```

```python
import functools

import jax
import jax.numpy as jnp
from jax import lax
from jax.experimental import pallas as pl
from jax.experimental.pallas import tpu as pltpu
from jax.sharding import PartitionSpec as P

HEAD_CHANNELS = 128
BLK = 128
NORM_EPS = 1e-06
CLAMP_LIMIT = 7.0
SIGMOID_SCALE = 1.702
MESH = pl.DeviceIdType.MESH
F32, BF16 = jnp.float32, jnp.bfloat16
VMEM = pl.BlockSpec(memory_space=pltpu.VMEM)
ANY = pl.BlockSpec(memory_space=pl.ANY)


def clamped_unit(gate_pre, up_pre):
    gate_pre = jnp.minimum(gate_pre, CLAMP_LIMIT)
    up_pre = jnp.clip(up_pre, -CLAMP_LIMIT, CLAMP_LIMIT)
    return (up_pre + 1.0) * gate_pre * jax.nn.sigmoid(SIGMOID_SCALE * gate_pre)


def dot(a, b, ca=1, cb=0):
    return lax.dot_general(a, b, (((ca,), (cb,)), ((), ())), preferred_element_type=F32)


def mixer_kernel(
    n_ep, q_ref, g_ref, v_ref, m_ref, pos_ref, gain_ref, w_ref, o_ref,
    q_in, inner, inc, dec, snd, got, send_sem, recv_sem,
):
    tokens, width = q_ref.shape
    heads, nblk = width // HEAD_CHANNELS, tokens // BLK
    me = lax.axis_index("ep")
    barrier = pltpu.get_barrier_semaphore()
    for k in range(1, n_ep):
        pl.semaphore_signal(
            barrier, inc=1, device_id={"ep": lax.rem(me + k, n_ep)}, device_id_type=MESH
        )

    row = lax.broadcasted_iota(jnp.int32, (BLK, BLK), 0)
    col = lax.broadcasted_iota(jnp.int32, (BLK, BLK), 1)
    masks = (row >= col, row <= col)
    floor = jnp.exp(m_ref[...])

    def cols(h):
        return slice(h * HEAD_CHANNELS, (h + 1) * HEAD_CHANNELS)

    def block_rows(b):
        return pl.ds(pl.multiple_of(b * BLK, BLK), BLK)

    def local(b, carry):
        rows = block_rows(b)
        q = q_ref[rows, :].astype(F32)
        q = q * jax.nn.sigmoid(q) * HEAD_CHANNELS ** (-0.5)
        shut = jax.nn.sigmoid(-g_ref[rows, :].astype(F32))
        v = v_ref[rows, :]
        pos_rows = pos_ref[rows, :]
        pos = jnp.concatenate(
            [jnp.broadcast_to(pos_rows[:, h : h + 1], (BLK, HEAD_CHANNELS)) for h in range(heads)],
            axis=1,
        )
        scores = [None] * heads
        for d in range(2):
            key = floor[d : d + 1, :] * shut
            rate = jnp.log1p(-key) + pos
            hi = rate.astype(BF16)
            lo = (rate - hi.astype(F32)).astype(BF16)
            tri = masks[d].astype(F32).astype(BF16)
            cumul = dot(tri, hi) + dot(tri, lo)
            last = cumul[BLK - 1 :, :] if d == 0 else cumul[:1, :]
            query_in = (q * jnp.exp(cumul)).astype(BF16)
            key_in = (key * jnp.exp(-cumul)).astype(BF16)
            key_state = (key * jnp.exp(last - cumul)).astype(BF16)
            q_in[d, rows, :] = query_in
            dec[b, d : d + 1, :] = jnp.exp(last)
            for h in range(heads):
                s = dot(query_in[:, cols(h)], key_in[:, cols(h)], 1, 1)
                s = jnp.where(masks[d], s, 0.0)
                scores[h] = s if d == 0 else scores[h] + s
                inc[d, b, :, cols(h)] = dot(v[:, cols(h)], key_state[:, cols(h)], 0, 0)
        for h in range(heads):
            inner[rows, cols(h)] = dot(scores[h].astype(BF16), v[:, cols(h)])
        return carry

    lax.fori_loop(0, nblk, local, 0)

    for d in range(2):
        def advance(i, carry, d=d):
            state, total = carry
            b = i if d == 0 else nblk - 1 - i
            decay = dec[b, d : d + 1, :]
            return state * decay + inc[d, b], total * decay

        state, total = lax.fori_loop(
            0, nblk, advance, (jnp.zeros((HEAD_CHANNELS, width), F32), jnp.ones((1, width), F32))
        )
        snd[d, :HEAD_CHANNELS, :] = state.astype(BF16)
        snd[d, HEAD_CHANNELS:, :] = jnp.broadcast_to(total, (16, width)).astype(BF16)

    pl.semaphore_wait(barrier, n_ep - 1)
    copies = []
    for k in range(1, n_ep):
        copy = pltpu.make_async_remote_copy(
            src_ref=snd,
            dst_ref=got.at[k],
            send_sem=send_sem.at[k],
            recv_sem=recv_sem.at[k],
            device_id={"ep": lax.rem(me + k, n_ep)},
            device_id_type=MESH,
        )
        copy.start()
        copies.append(copy)
    for copy in copies:
        copy.wait()

    entering = []
    for d in range(2):
        state = jnp.zeros((HEAD_CHANNELS, width), F32)
        for k in range(n_ep - 1, 0, -1):
            slot = k if d == 0 else n_ep - k
            valid = (me - k >= 0) if d == 0 else (me + k < n_ep)
            decay = got[slot, d, HEAD_CHANNELS:, :].astype(F32)[:1, :]
            new = state * decay + got[slot, d, :HEAD_CHANNELS, :].astype(F32)
            state = jnp.where(valid, new, state)
        entering.append(state)

    def ahead(b, state):
        rows = block_rows(b)
        low = state.astype(BF16)
        for h in range(heads):
            inner[rows, cols(h)] += dot(q_in[0, rows, cols(h)], low[:, cols(h)], 1, 1)
        return state * dec[b, 0:1, :] + inc[0, b]

    lax.fori_loop(0, nblk, ahead, entering[0])
    gain = gain_ref[...]

    def back(i, state):
        b = nblk - 1 - i
        rows = block_rows(b)
        low = state.astype(BF16)
        outs = []
        for h in range(heads):
            mix = inner[rows, cols(h)] + dot(q_in[1, rows, cols(h)], low[:, cols(h)], 1, 1)
            mean = jnp.mean(mix * mix, axis=-1, keepdims=True)
            outs.append((mix * lax.rsqrt(mean + NORM_EPS) * gain).astype(BF16))
        o_ref[rows, :] = dot(jnp.concatenate(outs, axis=1), w_ref[...]).astype(BF16)
        return state * dec[b, 1:2, :] + inc[1, b]

    lax.fori_loop(0, nblk, back, entering[1])


def mixer(n_ep, query, logits, value, margin, pos, gain, weight):
    tokens, width = query.shape
    features = weight.shape[1]
    nblk = tokens // BLK
    return pl.pallas_call(
        functools.partial(mixer_kernel, n_ep),
        out_shape=jax.ShapeDtypeStruct((tokens, features), BF16),
        in_specs=[VMEM] * 7,
        out_specs=VMEM,
        scratch_shapes=[
            pltpu.VMEM((2, tokens, width), BF16),
            pltpu.VMEM((tokens, width), F32),
            pltpu.VMEM((2, nblk, HEAD_CHANNELS, width), F32),
            pltpu.VMEM((nblk, 2, width), F32),
            pltpu.VMEM((2, HEAD_CHANNELS + 16, width), BF16),
            pltpu.VMEM((n_ep, 2, HEAD_CHANNELS + 16, width), BF16),
            pltpu.SemaphoreType.DMA((n_ep,)),
            pltpu.SemaphoreType.DMA((n_ep,)),
        ],
        compiler_params=pltpu.CompilerParams(
            collective_id=0, has_side_effects=True, vmem_limit_bytes=28 << 20
        ),
        cost_estimate=pl.CostEstimate(
            flops=20_000_000_000, bytes_accessed=8_000_000, transcendentals=0
        ),
        name="mixer",
    )(query, logits, value, margin, pos, gain, weight)


def expert_kernel(
    chunks, x_hbm, g_hbm, u_hbm, d_hbm, o_ref,
    x, wg, wu, wd, xc, xp, own, mid, to_c, from_c, to_d, from_d, to_p, from_p,
    load_sem, core_send, core_recv, link_send, link_recv,
):
    rows, features = x.shape
    n = rows // chunks
    t = lax.axis_index("tp")
    core = t + 1 - 2 * lax.rem(t, 2)
    peer = lax.rem(t + 2, 4)

    loads = [
        pltpu.make_async_copy(s, d, load_sem.at[i])
        for i, (s, d) in enumerate(((x_hbm, x), (g_hbm, wg), (u_hbm, wu), (d_hbm, wd)))
    ]
    for load in loads:
        load.start()
    barrier = pltpu.get_barrier_semaphore()
    for other in (core, peer):
        pl.semaphore_signal(barrier, inc=1, device_id={"tp": other}, device_id_type=MESH)
    pl.semaphore_wait(barrier, 2)

    def remote(src, dst, sends, recvs, index, other):
        return pltpu.make_async_remote_copy(
            src_ref=src,
            dst_ref=dst,
            send_sem=sends.at[index],
            recv_sem=recvs.at[index],
            device_id={"tp": other},
            device_id_type=MESH,
        )

    def mlp(block, store):
        hidden = clamped_unit(dot(block, wg[...]), dot(block, wu[...])).astype(BF16)
        step = 512 if features % 512 == 0 else features
        for at in range(0, features, step):
            store(slice(at, at + step), dot(hidden, wd[:, at : at + step]))

    def part(i):
        return pl.ds(i * n, n)

    loads[0].wait()
    gather = [
        remote(x.at[part(i)], xp.at[i, 0], link_send, link_recv, i, peer) for i in range(chunks)
    ]
    for copy in gather:
        copy.start()
    across = remote(x, xc, core_send, core_recv, 0, core)
    across.start()
    for load in loads[1:]:
        load.wait()

    def keep_own(at, value):
        own[:, at] = value

    mlp(x[...], keep_own)
    across.wait()

    def keep_core(at, value):
        to_c[:, at] = value.astype(BF16)

    mlp(xc[...], keep_core)
    give = remote(to_c, from_c, core_send, core_recv, 1, core)
    give.start()

    later = []
    for i in range(chunks):
        gather[i].wait_recv()
        forward = remote(xp.at[i, 0], xp.at[i, 1], core_send, core_recv, 2 + i, core)
        forward.start()
        forward.wait_recv()

        def keep_pair(at, value, i=i):
            mid[:, at] = value[:n]
            to_d[i, :, at] = value[n:].astype(BF16)

        mlp(xp[i].reshape(2 * n, features), keep_pair)
        swap = remote(to_d.at[i], from_d.at[i], core_send, core_recv, 2 + chunks + i, core)
        swap.start()
        swap.wait_recv()
        to_p[i] = (mid[...] + from_d[i].astype(F32)).astype(BF16)
        back = remote(to_p.at[i], from_p.at[i], link_send, link_recv, chunks + i, peer)
        back.start()
        later.append((forward, swap, back))

    give.wait_recv()
    for i in range(chunks):
        later[i][2].wait_recv()
        o_ref[part(i), :] = (
            own[part(i), :] + from_c[part(i), :].astype(F32) + from_p[i].astype(F32)
        ).astype(BF16)
    give.wait_send()
    for i in range(chunks):
        gather[i].wait_send()
        for copy in later[i]:
            copy.wait_send()


def experts(x, gate_weight, up_weight, down_weight):
    rows, features = x.shape
    hidden = gate_weight.shape[1]
    chunks = next(k for k in (3, 4, 2, 1) if rows % (16 * k) == 0 or k == 1)
    n = rows // chunks
    return pl.pallas_call(
        functools.partial(expert_kernel, chunks),
        out_shape=jax.ShapeDtypeStruct((rows, features), BF16),
        in_specs=[ANY] * 4,
        out_specs=VMEM,
        scratch_shapes=[
            pltpu.VMEM((rows, features), BF16),
            pltpu.VMEM((features, hidden), BF16),
            pltpu.VMEM((features, hidden), BF16),
            pltpu.VMEM((hidden, features), BF16),
            pltpu.VMEM((rows, features), BF16),
            pltpu.VMEM((chunks, 2, n, features), BF16),
            pltpu.VMEM((rows, features), F32),
            pltpu.VMEM((n, features), F32),
            pltpu.VMEM((rows, features), BF16),
            pltpu.VMEM((rows, features), BF16),
            pltpu.VMEM((chunks, n, features), BF16),
            pltpu.VMEM((chunks, n, features), BF16),
            pltpu.VMEM((chunks, n, features), BF16),
            pltpu.VMEM((chunks, n, features), BF16),
            pltpu.SemaphoreType.DMA((4,)),
            pltpu.SemaphoreType.DMA((2 + 2 * chunks,)),
            pltpu.SemaphoreType.DMA((2 + 2 * chunks,)),
            pltpu.SemaphoreType.DMA((2 * chunks,)),
            pltpu.SemaphoreType.DMA((2 * chunks,)),
        ],
        compiler_params=pltpu.CompilerParams(
            collective_id=1, has_side_effects=True, vmem_limit_bytes=48 << 20
        ),
        cost_estimate=pl.CostEstimate(
            flops=40_000_000_000, bytes_accessed=12_000_000, transcendentals=0
        ),
        name="experts",
    )(x, gate_weight, up_weight, down_weight)


def body(
    query,
    forget_gate_logits,
    value,
    forget_lower_margin,
    position_log_decay,
    head_norm_gain,
    mixer_output_weight,
    second_batch_tokens,
    expert_norm_gain,
    routes,
    chosen_expert_weight,
    gate_weight,
    up_weight,
    down_weight,
):
    tokens, top_count = routes.shape
    features = second_batch_tokens.shape[1]
    n_ep = lax.axis_size("ep")
    capacity = (3 * tokens * top_count + 2 * n_ep - 1) // (2 * n_ep)
    tokens_f = second_batch_tokens.astype(F32)
    normed = (
        tokens_f
        * lax.rsqrt(jnp.mean(tokens_f * tokens_f, axis=-1, keepdims=True) + NORM_EPS)
        * expert_norm_gain
    ).astype(BF16)
    named = routes[:, :, None] == jnp.arange(n_ep, dtype=jnp.int32)[None, None, :]
    chosen = jnp.any(named, axis=1)
    earlier = jnp.tril(jnp.ones((tokens, tokens), BF16), -1)
    ranking = dot(earlier, chosen.astype(BF16)).astype(jnp.int32)
    slot = jnp.where(named, ranking[:, None, :] + jnp.arange(n_ep) * capacity, 0)
    destination = jnp.sum(slot, axis=2)
    places = jnp.arange(n_ep * capacity, dtype=jnp.int32)
    hit = destination[:, :, None] == places
    pick = jnp.any(hit, axis=1).astype(BF16)
    share = jnp.sum(jnp.where(hit, chosen_expert_weight[:, :, None], 0.0), axis=1)
    share_hi = share.astype(BF16)
    share_lo = (share - share_hi.astype(F32)).astype(BF16)
    send = dot(pick, normed, 0, 0).astype(BF16)
    arrived = lax.all_to_all(send, "ep", split_axis=0, concat_axis=0, tiled=True)

    mixed = mixer(
        n_ep,
        query,
        forget_gate_logits,
        value,
        forget_lower_margin,
        jnp.transpose(position_log_decay),
        head_norm_gain[None, :],
        mixer_output_weight,
    )
    first_mixer_output = lax.psum_scatter(mixed, "tp", scatter_dimension=0, tiled=True)
    expert_sum = experts(arrived, gate_weight[0], up_weight[0], down_weight[0])
    returned = lax.all_to_all(expert_sum, "ep", split_axis=0, concat_axis=0, tiled=True)
    moe_out = (dot(share_hi, returned) + dot(share_lo, returned)).astype(BF16)
    return (first_mixer_output, moe_out)


def solution(mesh):
    return jax.shard_map(
        body,
        mesh=mesh,
        in_specs=(
            P(("grp", "ep"), "tp"),
            P(("grp", "ep"), "tp"),
            P(("grp", "ep"), "tp"),
            P(None, "tp"),
            P("tp", ("grp", "ep")),
            P(),
            P("tp", None),
            P(("grp", "ep", "tp"), None),
            P(),
            P(("grp", "ep", "tp"), None),
            P(("grp", "ep", "tp"), None),
            P("ep", None, "tp"),
            P("ep", None, "tp"),
            P("ep", "tp", None),
        ),
        out_specs=(P(("grp", "ep", "tp"), None), P(("grp", "ep", "tp"), None)),
        check_vma=False,
    )
```

```python
import functools

import jax
import jax.numpy as jnp
from jax import lax
from jax.experimental import pallas as pl
from jax.experimental.pallas import tpu as pltpu
from jax.sharding import PartitionSpec as P

HEAD_CHANNELS = 128
BLK = 128
NORM_EPS = 1e-06
CLAMP_LIMIT = 7.0
SIGMOID_SCALE = 1.702
MESH = pl.DeviceIdType.MESH
F32, BF16 = jnp.float32, jnp.bfloat16
VMEM = pl.BlockSpec(memory_space=pltpu.VMEM)
ANY = pl.BlockSpec(memory_space=pl.ANY)


def clamped_unit(gate_pre, up_pre):
    gate_pre = jnp.minimum(gate_pre, CLAMP_LIMIT)
    up_pre = jnp.clip(up_pre, -CLAMP_LIMIT, CLAMP_LIMIT)
    return (up_pre + 1.0) * gate_pre * jax.nn.sigmoid(SIGMOID_SCALE * gate_pre)


def dot(a, b, ca=1, cb=0):
    return lax.dot_general(a, b, (((ca,), (cb,)), ((), ())), preferred_element_type=F32)


def fused_kernel(
    n_ep, chunks, q_ref, g_ref, v_ref, m_ref, pos_ref, gain_ref, w_ref, rows_ref, hi_ref, lo_ref,
    gate_hbm, up_hbm, down_hbm, mix_ref, moe_ref,
    q_in, inner, inc, dec, snd, got, mixed,
    wg, wu, wd, x, xc, xp, own, mid, to_c, from_c, to_d, from_d, to_p, from_p,
    ret, mix_c, mix_d, mix_r,
    load_sem, state_send, state_recv, slot_send, slot_recv, ret_send, ret_recv,
    core_send, core_recv, link_send, link_recv,
):
    tokens, width = q_ref.shape
    heads, nblk = width // HEAD_CHANNELS, tokens // BLK
    rows, features = x.shape
    capacity, n = rows // n_ep, rows // chunks
    per = n_ep // chunks
    share = tokens // 4
    me = lax.axis_index("ep")
    t = lax.axis_index("tp")
    core = t + 1 - 2 * lax.rem(t, 2)
    peer = lax.rem(t + 2, 4)
    diag = lax.rem(core + 2, 4)

    loads = [
        pltpu.make_async_copy(s, d, load_sem.at[i])
        for i, (s, d) in enumerate(((gate_hbm, wg), (up_hbm, wu), (down_hbm, wd)))
    ]
    barrier = pltpu.get_barrier_semaphore()
    for k in range(1, n_ep):
        pl.semaphore_signal(
            barrier, inc=1, device_id={"ep": lax.rem(me + k, n_ep)}, device_id_type=MESH
        )
    for other in (core, peer):
        pl.semaphore_signal(barrier, inc=1, device_id={"tp": other}, device_id_type=MESH)
    for load in loads:
        load.start()
    pl.semaphore_wait(barrier, n_ep + 1)

    def remote(src, dst, sends, recvs, index, axis, other):
        return pltpu.make_async_remote_copy(
            src_ref=src,
            dst_ref=dst,
            send_sem=sends.at[index],
            recv_sem=recvs.at[index],
            device_id={axis: other},
            device_id_type=MESH,
        )

    def slot(k):
        return pl.ds(k * capacity, capacity)

    def part(i):
        return pl.ds(i * n, n)

    def to_core(src, dst, index):
        return remote(src, dst, core_send, core_recv, index, "tp", core)

    def to_peer(src, dst, index):
        return remote(src, dst, link_send, link_recv, index, "tp", peer)

    unsent = []
    stay = pltpu.make_async_copy(rows_ref.at[slot(0)], x.at[slot(0)], load_sem.at[3])
    stay.start()
    dispatch = [None]
    for k in range(1, n_ep):
        copy = remote(
            rows_ref.at[slot(k)], x.at[slot(k)], slot_send, slot_recv, k, "ep",
            lax.rem(me + k, n_ep),
        )
        copy.start()
        dispatch.append(copy)
        unsent.append(copy)
    stay.wait()

    gather, across = [], []

    def share_chunk(i):
        for k in range(i * per, (i + 1) * per):
            if k > 0:
                dispatch[k].wait_recv()
        copy = to_peer(x.at[part(i)], xp.at[i, 0], i)
        copy.start()
        gather.append(copy)
        unsent.append(copy)
        copy = to_core(x.at[part(i)], xc.at[part(i)], i)
        copy.start()
        across.append(copy)
        unsent.append(copy)

    share_chunk(0)

    row = lax.broadcasted_iota(jnp.int32, (BLK, BLK), 0)
    col = lax.broadcasted_iota(jnp.int32, (BLK, BLK), 1)
    masks = (row >= col, row <= col)
    floor = jnp.exp(m_ref[...])

    def cols(h):
        return slice(h * HEAD_CHANNELS, (h + 1) * HEAD_CHANNELS)

    def block_rows(b):
        return pl.ds(pl.multiple_of(b * BLK, BLK), BLK)

    def local(b, carry):
        rows = block_rows(b)
        q = q_ref[rows, :].astype(F32)
        q = q * jax.nn.sigmoid(q) * HEAD_CHANNELS ** (-0.5)
        shut = jax.nn.sigmoid(-g_ref[rows, :].astype(F32))
        v = v_ref[rows, :]
        pos_rows = pos_ref[rows, :]
        pos = jnp.concatenate(
            [jnp.broadcast_to(pos_rows[:, h : h + 1], (BLK, HEAD_CHANNELS)) for h in range(heads)],
            axis=1,
        )
        scores = [None] * heads
        for d in range(2):
            key = floor[d : d + 1, :] * shut
            rate = jnp.log1p(-key) + pos
            hi = rate.astype(BF16)
            lo = (rate - hi.astype(F32)).astype(BF16)
            tri = masks[d].astype(F32).astype(BF16)
            cumul = dot(tri, hi) + dot(tri, lo)
            last = cumul[BLK - 1 :, :] if d == 0 else cumul[:1, :]
            query_in = (q * jnp.exp(cumul)).astype(BF16)
            key_in = (key * jnp.exp(-cumul)).astype(BF16)
            key_state = (key * jnp.exp(last - cumul)).astype(BF16)
            q_in[d, rows, :] = query_in
            dec[b, d : d + 1, :] = jnp.exp(last)
            for h in range(heads):
                s = dot(query_in[:, cols(h)], key_in[:, cols(h)], 1, 1)
                s = jnp.where(masks[d], s, 0.0)
                scores[h] = s if d == 0 else scores[h] + s
                inc[d, b, :, cols(h)] = dot(v[:, cols(h)], key_state[:, cols(h)], 0, 0)
        for h in range(heads):
            inner[rows, cols(h)] = dot(scores[h].astype(BF16), v[:, cols(h)])
        return carry

    half = nblk // 2
    lax.fori_loop(0, half, local, 0)
    if chunks > 1:
        share_chunk(1)
    lax.fori_loop(half, nblk, local, 0)

    for d in range(2):
        def advance(i, carry, d=d):
            state, total = carry
            b = i if d == 0 else nblk - 1 - i
            decay = dec[b, d : d + 1, :]
            return state * decay + inc[d, b], total * decay

        state, total = lax.fori_loop(
            0, nblk, advance, (jnp.zeros((HEAD_CHANNELS, width), F32), jnp.ones((1, width), F32))
        )
        snd[d, :HEAD_CHANNELS, :] = state.astype(BF16)
        snd[d, HEAD_CHANNELS:, :] = jnp.broadcast_to(total, (16, width)).astype(BF16)

    states = []
    for k in range(1, n_ep):
        copy = remote(
            snd, got.at[k], state_send, state_recv, k, "ep", lax.rem(me + k, n_ep)
        )
        copy.start()
        states.append(copy)
        unsent.append(copy)
    for i in range(2, chunks):
        share_chunk(i)

    def mlp(block, store):
        hidden = clamped_unit(dot(block, wg[...]), dot(block, wu[...])).astype(BF16)
        step = 512 if features % 512 == 0 else features
        for at in range(0, features, step):
            store(slice(at, at + step), dot(hidden, wd[:, at : at + step]))

    for load in loads:
        load.wait()

    def keep_own(at, value):
        own[:, at] = value

    mlp(x[...], keep_own)

    def keep_core(at, value):
        to_c[:, at] = value.astype(BF16)

    for copy in across:
        copy.wait_recv()
    mlp(xc[...], keep_core)
    give = to_core(to_c, from_c, chunks)
    give.start()

    for copy in states:
        copy.wait_recv()
    entering = []
    for d in range(2):
        state = jnp.zeros((HEAD_CHANNELS, width), F32)
        for k in range(n_ep - 1, 0, -1):
            at = k if d == 0 else n_ep - k
            valid = (me - k >= 0) if d == 0 else (me + k < n_ep)
            decay = got[at, d, HEAD_CHANNELS:, :].astype(F32)[:1, :]
            new = state * decay + got[at, d, :HEAD_CHANNELS, :].astype(F32)
            state = jnp.where(valid, new, state)
        entering.append(state)

    def ahead(b, state):
        rows = block_rows(b)
        low = state.astype(BF16)
        for h in range(heads):
            inner[rows, cols(h)] += dot(q_in[0, rows, cols(h)], low[:, cols(h)], 1, 1)
        return state * dec[b, 0:1, :] + inc[0, b]

    lax.fori_loop(0, nblk, ahead, entering[0])
    gain = gain_ref[...]

    def back(i, state):
        b = nblk - 1 - i
        rows = block_rows(b)
        low = state.astype(BF16)
        outs = []
        for h in range(heads):
            mix = inner[rows, cols(h)] + dot(q_in[1, rows, cols(h)], low[:, cols(h)], 1, 1)
            mean = jnp.mean(mix * mix, axis=-1, keepdims=True)
            outs.append((mix * lax.rsqrt(mean + NORM_EPS) * gain).astype(BF16))
        mixed[rows, :] = dot(jnp.concatenate(outs, axis=1), w_ref[...]).astype(BF16)
        return state * dec[b, 1:2, :] + inc[1, b]

    lax.fori_loop(0, nblk, back, entering[1])

    def rows_of(owner):
        return pl.ds(owner * share, share)

    mix_give = to_core(mixed.at[rows_of(core)], mix_c, chunks + 1)
    mix_swap = to_core(mixed.at[rows_of(diag)], mix_d, chunks + 2)
    base = chunks + 3
    forwards = []
    for i in range(chunks):
        gather[i].wait_recv()
        copy = to_core(xp.at[i, 0], xp.at[i, 1], base + i)
        copy.start()
        forwards.append(copy)
        unsent.append(copy)
    for copy in (mix_swap, mix_give):
        copy.start()
        unsent.append(copy)

    backs = []
    for i in range(chunks):
        forwards[i].wait_recv()

        def keep_pair(at, value, i=i):
            mid[:, at] = value[:n]
            to_d[i, :, at] = value[n:].astype(BF16)

        mlp(xp[i].reshape(2 * n, features), keep_pair)
        swap = to_core(to_d.at[i], from_d.at[i], base + chunks + i)
        swap.start()
        unsent.append(swap)
        swap.wait_recv()
        to_p[i] = (mid[...] + from_d[i].astype(F32)).astype(BF16)
        copy = to_peer(to_p.at[i], from_p.at[i], chunks + i)
        copy.start()
        backs.append(copy)
        unsent.append(copy)

    mix_swap.wait_recv()
    mix_d[...] = (mixed[rows_of(peer), :].astype(F32) + mix_d[...].astype(F32)).astype(BF16)
    mix_back = to_peer(mix_d, mix_r, 2 * chunks)
    mix_back.start()
    unsent.append(mix_back)

    give.wait()
    out = to_c
    returns = []
    for i in range(chunks):
        backs[i].wait_recv()
        out[part(i), :] = (
            own[part(i), :] + from_c[part(i), :].astype(F32) + from_p[i].astype(F32)
        ).astype(BF16)
        for k in range(i * per, (i + 1) * per):
            if k == 0:
                stay = pltpu.make_async_copy(out.at[slot(0)], ret.at[slot(0)], load_sem.at[3])
                stay.start()
            else:
                copy = remote(
                    out.at[slot(k)], ret.at[slot(k)], ret_send, ret_recv, k, "ep",
                    lax.rem(me + n_ep - k, n_ep),
                )
                copy.start()
                returns.append(copy)
                unsent.append(copy)

    mix_give.wait_recv()
    mix_back.wait_recv()
    mix_ref[...] = (
        mixed[rows_of(t), :].astype(F32) + mix_c[...].astype(F32) + mix_r[...].astype(F32)
    ).astype(BF16)
    stay.wait()
    for copy in returns:
        copy.wait_recv()
    step = 512 if features % 512 == 0 else features
    for at in range(0, features, step):
        block = ret[:, at : at + step]
        moe_ref[:, at : at + step] = (
            dot(hi_ref[...], block) + dot(lo_ref[...], block)
        ).astype(BF16)
    for copy in unsent:
        copy.wait_send()


def fused(n_ep, query, logits, value, margin, pos, gain, weight, send, hi, lo, gate, up, down):
    tokens, width = query.shape
    rows, features = send.shape
    hidden = gate.shape[1]
    nblk, share = tokens // BLK, tokens // 4
    chunks = 4 if n_ep % 4 == 0 else n_ep
    n = rows // chunks
    dma = pltpu.SemaphoreType.DMA

    def low(*shape):
        return pltpu.VMEM(shape, BF16)

    return pl.pallas_call(
        functools.partial(fused_kernel, n_ep, chunks),
        out_shape=(
            jax.ShapeDtypeStruct((share, features), BF16),
            jax.ShapeDtypeStruct((hi.shape[0], features), BF16),
        ),
        in_specs=[VMEM] * 10 + [ANY] * 3,
        out_specs=(VMEM, VMEM),
        scratch_shapes=[
            low(2, tokens, width),
            pltpu.VMEM((tokens, width), F32),
            pltpu.VMEM((2, nblk, HEAD_CHANNELS, width), F32),
            pltpu.VMEM((nblk, 2, width), F32),
            low(2, HEAD_CHANNELS + 16, width),
            low(n_ep, 2, HEAD_CHANNELS + 16, width),
            low(tokens, features),
            low(features, hidden),
            low(features, hidden),
            low(hidden, features),
            low(rows, features),
            low(rows, features),
            low(chunks, 2, n, features),
            pltpu.VMEM((rows, features), F32),
            pltpu.VMEM((n, features), F32),
            low(rows, features),
            low(rows, features),
            low(chunks, n, features),
            low(chunks, n, features),
            low(chunks, n, features),
            low(chunks, n, features),
            low(rows, features),
            low(share, features),
            low(share, features),
            low(share, features),
            dma((4,)),
            dma((n_ep,)),
            dma((n_ep,)),
            dma((n_ep,)),
            dma((n_ep,)),
            dma((n_ep,)),
            dma((n_ep,)),
            dma((3 * chunks + 3,)),
            dma((3 * chunks + 3,)),
            dma((2 * chunks + 1,)),
            dma((2 * chunks + 1,)),
        ],
        compiler_params=pltpu.CompilerParams(
            collective_id=0, has_side_effects=True, vmem_limit_bytes=61 << 20
        ),
        name="fused",
    )(query, logits, value, margin, pos, gain, weight, send, hi, lo, gate, up, down)


def body(
    query,
    forget_gate_logits,
    value,
    forget_lower_margin,
    position_log_decay,
    head_norm_gain,
    mixer_output_weight,
    second_batch_tokens,
    expert_norm_gain,
    routes,
    chosen_expert_weight,
    gate_weight,
    up_weight,
    down_weight,
):
    tokens, top_count = routes.shape
    features = second_batch_tokens.shape[1]
    n_ep = lax.axis_size("ep")
    capacity = (3 * tokens * top_count + 2 * n_ep - 1) // (2 * n_ep)
    capacity = -(-capacity // 16) * 16
    tokens_f = second_batch_tokens.astype(F32)
    normed = (
        tokens_f
        * lax.rsqrt(jnp.mean(tokens_f * tokens_f, axis=-1, keepdims=True) + NORM_EPS)
        * expert_norm_gain
    ).astype(BF16)
    ahead = jnp.mod(routes - lax.axis_index("ep"), n_ep)
    named = ahead[:, :, None] == jnp.arange(n_ep, dtype=jnp.int32)[None, None, :]
    chosen = jnp.any(named, axis=1)
    earlier = jnp.tril(jnp.ones((tokens, tokens), BF16), -1)
    ranking = dot(earlier, chosen.astype(BF16)).astype(jnp.int32)
    slot = jnp.where(named, ranking[:, None, :] + jnp.arange(n_ep) * capacity, 0)
    destination = jnp.sum(slot, axis=2)
    places = jnp.arange(n_ep * capacity, dtype=jnp.int32)
    hit = destination[:, :, None] == places
    pick = jnp.any(hit, axis=1).astype(BF16)
    share = jnp.sum(jnp.where(hit, chosen_expert_weight[:, :, None], 0.0), axis=1)
    share_hi = share.astype(BF16)
    share_lo = (share - share_hi.astype(F32)).astype(BF16)
    send = dot(pick, normed, 0, 0).astype(BF16)
    return fused(
        n_ep,
        query,
        forget_gate_logits,
        value,
        forget_lower_margin,
        jnp.transpose(position_log_decay),
        head_norm_gain[None, :],
        mixer_output_weight,
        send,
        share_hi,
        share_lo,
        gate_weight[0],
        up_weight[0],
        down_weight[0],
    )


def solution(mesh):
    return jax.shard_map(
        body,
        mesh=mesh,
        in_specs=(
            P(("grp", "ep"), "tp"),
            P(("grp", "ep"), "tp"),
            P(("grp", "ep"), "tp"),
            P(None, "tp"),
            P("tp", ("grp", "ep")),
            P(),
            P("tp", None),
            P(("grp", "ep", "tp"), None),
            P(),
            P(("grp", "ep", "tp"), None),
            P(("grp", "ep", "tp"), None),
            P("ep", None, "tp"),
            P("ep", None, "tp"),
            P("ep", "tp", None),
        ),
        out_specs=(P(("grp", "ep", "tp"), None), P(("grp", "ep", "tp"), None)),
        check_vma=False,
    )
```

```python
import functools

import jax
import jax.numpy as jnp
from jax import lax
from jax.experimental import pallas as pl
from jax.experimental.pallas import tpu as pltpu
from jax.sharding import PartitionSpec as P

HEAD_CHANNELS = 128
BLK = 128
NORM_EPS = 1e-06
CLAMP_LIMIT = 7.0
SIGMOID_SCALE = 1.702
MESH = pl.DeviceIdType.MESH
F32, BF16 = jnp.float32, jnp.bfloat16
VMEM = pl.BlockSpec(memory_space=pltpu.VMEM)
ANY = pl.BlockSpec(memory_space=pl.ANY)


def clamped_unit(gate_pre, up_pre):
    gate_pre = jnp.minimum(gate_pre, CLAMP_LIMIT)
    up_pre = jnp.clip(up_pre, -CLAMP_LIMIT, CLAMP_LIMIT)
    return (up_pre + 1.0) * gate_pre * jax.nn.sigmoid(SIGMOID_SCALE * gate_pre)


def dot(a, b, ca=1, cb=0):
    return lax.dot_general(a, b, (((ca,), (cb,)), ((), ())), preferred_element_type=F32)


def fused_kernel(
    n_ep, chunks, q_ref, g_ref, v_ref, m_ref, pos_ref, gain_ref, w_ref, rows_ref, hi_ref, lo_ref,
    gate_hbm, up_hbm, down_hbm, mix_ref, moe_ref,
    q_in, inner, inc, dec, snd, got, mixed,
    wg, wu, wd, x, xc, xp, own, mid, to_c, from_c, to_d, from_d, to_p, from_p,
    ret, mix_c, mix_d, mix_r,
    load_sem, state_send, state_recv, slot_send, slot_recv, ret_send, ret_recv,
    core_send, core_recv, link_send, link_recv,
):
    tokens, width = q_ref.shape
    heads, nblk = width // HEAD_CHANNELS, tokens // BLK
    rows, features = x.shape
    capacity, n = rows // n_ep, rows // chunks
    per = n_ep // chunks
    share = tokens // 4
    me = lax.axis_index("ep")
    t = lax.axis_index("tp")
    core = t + 1 - 2 * lax.rem(t, 2)
    peer = lax.rem(t + 2, 4)
    diag = lax.rem(core + 2, 4)

    loads = [
        pltpu.make_async_copy(s, d, load_sem.at[i])
        for i, (s, d) in enumerate(((gate_hbm, wg), (up_hbm, wu), (down_hbm, wd)))
    ]
    barrier = pltpu.get_barrier_semaphore()
    for k in range(1, n_ep):
        pl.semaphore_signal(
            barrier, inc=1, device_id={"ep": lax.rem(me + k, n_ep)}, device_id_type=MESH
        )
    for other in (core, peer):
        pl.semaphore_signal(barrier, inc=1, device_id={"tp": other}, device_id_type=MESH)
    for load in loads:
        load.start()
    pl.semaphore_wait(barrier, n_ep + 1)

    def remote(src, dst, sends, recvs, index, axis, other):
        return pltpu.make_async_remote_copy(
            src_ref=src,
            dst_ref=dst,
            send_sem=sends.at[index],
            recv_sem=recvs.at[index],
            device_id={axis: other},
            device_id_type=MESH,
        )

    def slot(k):
        return pl.ds(k * capacity, capacity)

    def part(i):
        return pl.ds(i * n, n)

    def to_core(src, dst, index):
        return remote(src, dst, core_send, core_recv, index, "tp", core)

    def to_peer(src, dst, index):
        return remote(src, dst, link_send, link_recv, index, "tp", peer)

    unsent = []
    stay = pltpu.make_async_copy(rows_ref.at[slot(0)], x.at[slot(0)], load_sem.at[3])
    stay.start()
    dispatch = [None]
    for k in range(1, n_ep):
        copy = remote(
            rows_ref.at[slot(k)], x.at[slot(k)], slot_send, slot_recv, k, "ep",
            lax.rem(me + k, n_ep),
        )
        copy.start()
        dispatch.append(copy)
        unsent.append(copy)
    stay.wait()

    gather, across = [], []

    def share_chunk(i):
        for k in range(i * per, (i + 1) * per):
            if k > 0:
                dispatch[k].wait_recv()
        copy = to_peer(x.at[part(i)], xp.at[i, 0], i)
        copy.start()
        gather.append(copy)
        unsent.append(copy)
        copy = to_core(x.at[part(i)], xc.at[part(i)], i)
        copy.start()
        across.append(copy)
        unsent.append(copy)

    share_chunk(0)

    row = lax.broadcasted_iota(jnp.int32, (BLK, BLK), 0)
    col = lax.broadcasted_iota(jnp.int32, (BLK, BLK), 1)
    masks = (row >= col, row <= col)
    floor = jnp.exp(m_ref[...])

    def cols(h):
        return slice(h * HEAD_CHANNELS, (h + 1) * HEAD_CHANNELS)

    def block_rows(b):
        return pl.ds(pl.multiple_of(b * BLK, BLK), BLK)

    def local(b, carry):
        rows = block_rows(b)
        q = q_ref[rows, :].astype(F32)
        q = q * jax.nn.sigmoid(q) * HEAD_CHANNELS ** (-0.5)
        shut = jax.nn.sigmoid(-g_ref[rows, :].astype(F32))
        v = v_ref[rows, :]
        pos_rows = pos_ref[rows, :]
        pos = jnp.concatenate(
            [jnp.broadcast_to(pos_rows[:, h : h + 1], (BLK, HEAD_CHANNELS)) for h in range(heads)],
            axis=1,
        )
        scores = [None] * heads
        for d in range(2):
            key = floor[d : d + 1, :] * shut
            rate = jnp.log1p(-key) + pos
            hi = rate.astype(BF16)
            lo = (rate - hi.astype(F32)).astype(BF16)
            tri = masks[d].astype(F32).astype(BF16)
            cumul = dot(tri, hi) + dot(tri, lo)
            last = cumul[BLK - 1 :, :] if d == 0 else cumul[:1, :]
            query_in = (q * jnp.exp(cumul)).astype(BF16)
            key_in = (key * jnp.exp(-cumul)).astype(BF16)
            key_state = (key * jnp.exp(last - cumul)).astype(BF16)
            q_in[d, rows, :] = query_in
            dec[b, d : d + 1, :] = jnp.exp(last)
            for h in range(heads):
                s = dot(query_in[:, cols(h)], key_in[:, cols(h)], 1, 1)
                s = jnp.where(masks[d], s, 0.0)
                scores[h] = s if d == 0 else scores[h] + s
                inc[d, b, :, cols(h)] = dot(v[:, cols(h)], key_state[:, cols(h)], 0, 0)
        for h in range(heads):
            inner[rows, cols(h)] = dot(scores[h].astype(BF16), v[:, cols(h)])
        return carry

    half = nblk // 2
    lax.fori_loop(0, half, local, 0)
    if chunks > 1:
        share_chunk(1)
    lax.fori_loop(half, nblk, local, 0)

    for d in range(2):
        def advance(i, carry, d=d):
            state, total = carry
            b = i if d == 0 else nblk - 1 - i
            decay = dec[b, d : d + 1, :]
            return state * decay + inc[d, b], total * decay

        state, total = lax.fori_loop(
            0, nblk, advance, (jnp.zeros((HEAD_CHANNELS, width), F32), jnp.ones((1, width), F32))
        )
        snd[d, :HEAD_CHANNELS, :] = state.astype(BF16)
        snd[d, HEAD_CHANNELS:, :] = jnp.broadcast_to(total, (16, width)).astype(BF16)

    states = []
    for k in range(1, n_ep):
        copy = remote(
            snd, got.at[k], state_send, state_recv, k, "ep", lax.rem(me + k, n_ep)
        )
        copy.start()
        states.append(copy)
        unsent.append(copy)
    def mlp(block, store):
        hidden = clamped_unit(dot(block, wg[...]), dot(block, wu[...])).astype(BF16)
        step = 512 if features % 512 == 0 else features
        for at in range(0, features, step):
            store(slice(at, at + step), dot(hidden, wd[:, at : at + step]))

    for load in loads:
        load.wait()

    base = chunks + 3
    forwards, backs = [], []

    def forward_chunk(i):
        gather[i].wait_recv()
        copy = to_core(xp.at[i, 0], xp.at[i, 1], base + i)
        copy.start()
        forwards.append(copy)
        unsent.append(copy)

    def expert_chunk(i):
        forwards[i].wait_recv()

        def keep_pair(at, value):
            mid[:, at] = value[:n]
            to_d[i, :, at] = value[n:].astype(BF16)

        mlp(xp[i].reshape(2 * n, features), keep_pair)
        swap = to_core(to_d.at[i], from_d.at[i], base + chunks + i)
        swap.start()
        unsent.append(swap)
        swap.wait_recv()
        to_p[i] = (mid[...] + from_d[i].astype(F32)).astype(BF16)
        copy = to_peer(to_p.at[i], from_p.at[i], chunks + i)
        copy.start()
        backs.append(copy)
        unsent.append(copy)

    early = max(chunks - 2, 0)
    for i in range(early):
        share_chunk(i + 2)
        forward_chunk(i)
        expert_chunk(i)

    def keep_own(at, value):
        own[:, at] = value

    mlp(x[...], keep_own)

    def keep_core(at, value):
        to_c[:, at] = value.astype(BF16)

    for copy in across:
        copy.wait_recv()
    mlp(xc[...], keep_core)
    give = to_core(to_c, from_c, chunks)
    give.start()

    for copy in states:
        copy.wait_recv()
    entering = []
    for d in range(2):
        state = jnp.zeros((HEAD_CHANNELS, width), F32)
        for k in range(n_ep - 1, 0, -1):
            at = k if d == 0 else n_ep - k
            valid = (me - k >= 0) if d == 0 else (me + k < n_ep)
            decay = got[at, d, HEAD_CHANNELS:, :].astype(F32)[:1, :]
            new = state * decay + got[at, d, :HEAD_CHANNELS, :].astype(F32)
            state = jnp.where(valid, new, state)
        entering.append(state)

    def ahead(b, state):
        rows = block_rows(b)
        low = state.astype(BF16)
        for h in range(heads):
            inner[rows, cols(h)] += dot(q_in[0, rows, cols(h)], low[:, cols(h)], 1, 1)
        return state * dec[b, 0:1, :] + inc[0, b]

    lax.fori_loop(0, nblk, ahead, entering[0])
    gain = gain_ref[...]

    def back(i, state):
        b = nblk - 1 - i
        rows = block_rows(b)
        low = state.astype(BF16)
        outs = []
        for h in range(heads):
            mix = inner[rows, cols(h)] + dot(q_in[1, rows, cols(h)], low[:, cols(h)], 1, 1)
            mean = jnp.mean(mix * mix, axis=-1, keepdims=True)
            outs.append((mix * lax.rsqrt(mean + NORM_EPS) * gain).astype(BF16))
        mixed[rows, :] = dot(jnp.concatenate(outs, axis=1), w_ref[...]).astype(BF16)
        return state * dec[b, 1:2, :] + inc[1, b]

    lax.fori_loop(0, nblk, back, entering[1])

    def rows_of(owner):
        return pl.ds(owner * share, share)

    mix_give = to_core(mixed.at[rows_of(core)], mix_c, chunks + 1)
    mix_swap = to_core(mixed.at[rows_of(diag)], mix_d, chunks + 2)
    for i in range(early, chunks):
        forward_chunk(i)
    for copy in (mix_swap, mix_give):
        copy.start()
        unsent.append(copy)
    for i in range(early, chunks):
        expert_chunk(i)

    mix_swap.wait_recv()
    mix_d[...] = (mixed[rows_of(peer), :].astype(F32) + mix_d[...].astype(F32)).astype(BF16)
    mix_back = to_peer(mix_d, mix_r, 2 * chunks)
    mix_back.start()
    unsent.append(mix_back)

    give.wait()
    out = to_c
    returns = []
    for i in range(chunks):
        backs[i].wait_recv()
        out[part(i), :] = (
            own[part(i), :] + from_c[part(i), :].astype(F32) + from_p[i].astype(F32)
        ).astype(BF16)
        for k in range(i * per, (i + 1) * per):
            if k == 0:
                stay = pltpu.make_async_copy(out.at[slot(0)], ret.at[slot(0)], load_sem.at[3])
                stay.start()
            else:
                copy = remote(
                    out.at[slot(k)], ret.at[slot(k)], ret_send, ret_recv, k, "ep",
                    lax.rem(me + n_ep - k, n_ep),
                )
                copy.start()
                returns.append(copy)
                unsent.append(copy)

    mix_give.wait_recv()
    mix_back.wait_recv()
    mix_ref[...] = (
        mixed[rows_of(t), :].astype(F32) + mix_c[...].astype(F32) + mix_r[...].astype(F32)
    ).astype(BF16)
    stay.wait()
    for copy in returns:
        copy.wait_recv()
    step = 512 if features % 512 == 0 else features
    for at in range(0, features, step):
        block = ret[:, at : at + step]
        moe_ref[:, at : at + step] = (
            dot(hi_ref[...], block) + dot(lo_ref[...], block)
        ).astype(BF16)
    for copy in unsent:
        copy.wait_send()


def fused(n_ep, query, logits, value, margin, pos, gain, weight, send, hi, lo, gate, up, down):
    tokens, width = query.shape
    rows, features = send.shape
    hidden = gate.shape[1]
    nblk, share = tokens // BLK, tokens // 4
    chunks = 4 if n_ep % 4 == 0 else n_ep
    n = rows // chunks
    dma = pltpu.SemaphoreType.DMA

    def low(*shape):
        return pltpu.VMEM(shape, BF16)

    return pl.pallas_call(
        functools.partial(fused_kernel, n_ep, chunks),
        out_shape=(
            jax.ShapeDtypeStruct((share, features), BF16),
            jax.ShapeDtypeStruct((hi.shape[0], features), BF16),
        ),
        in_specs=[VMEM] * 10 + [ANY] * 3,
        out_specs=(VMEM, VMEM),
        scratch_shapes=[
            low(2, tokens, width),
            pltpu.VMEM((tokens, width), F32),
            pltpu.VMEM((2, nblk, HEAD_CHANNELS, width), F32),
            pltpu.VMEM((nblk, 2, width), F32),
            low(2, HEAD_CHANNELS + 16, width),
            low(n_ep, 2, HEAD_CHANNELS + 16, width),
            low(tokens, features),
            low(features, hidden),
            low(features, hidden),
            low(hidden, features),
            low(rows, features),
            low(rows, features),
            low(chunks, 2, n, features),
            pltpu.VMEM((rows, features), F32),
            pltpu.VMEM((n, features), F32),
            low(rows, features),
            low(rows, features),
            low(chunks, n, features),
            low(chunks, n, features),
            low(chunks, n, features),
            low(chunks, n, features),
            low(rows, features),
            low(share, features),
            low(share, features),
            low(share, features),
            dma((4,)),
            dma((n_ep,)),
            dma((n_ep,)),
            dma((n_ep,)),
            dma((n_ep,)),
            dma((n_ep,)),
            dma((n_ep,)),
            dma((3 * chunks + 3,)),
            dma((3 * chunks + 3,)),
            dma((2 * chunks + 1,)),
            dma((2 * chunks + 1,)),
        ],
        compiler_params=pltpu.CompilerParams(
            collective_id=0, has_side_effects=True, vmem_limit_bytes=61 << 20
        ),
        name="fused",
    )(query, logits, value, margin, pos, gain, weight, send, hi, lo, gate, up, down)


def body(
    query,
    forget_gate_logits,
    value,
    forget_lower_margin,
    position_log_decay,
    head_norm_gain,
    mixer_output_weight,
    second_batch_tokens,
    expert_norm_gain,
    routes,
    chosen_expert_weight,
    gate_weight,
    up_weight,
    down_weight,
):
    tokens, top_count = routes.shape
    features = second_batch_tokens.shape[1]
    n_ep = lax.axis_size("ep")
    capacity = (3 * tokens * top_count + 2 * n_ep - 1) // (2 * n_ep)
    capacity = -(-capacity // 16) * 16
    tokens_f = second_batch_tokens.astype(F32)
    normed = (
        tokens_f
        * lax.rsqrt(jnp.mean(tokens_f * tokens_f, axis=-1, keepdims=True) + NORM_EPS)
        * expert_norm_gain
    ).astype(BF16)
    ahead = jnp.mod(routes - lax.axis_index("ep"), n_ep)
    named = ahead[:, :, None] == jnp.arange(n_ep, dtype=jnp.int32)[None, None, :]
    chosen = jnp.any(named, axis=1)
    earlier = jnp.tril(jnp.ones((tokens, tokens), BF16), -1)
    ranking = dot(earlier, chosen.astype(BF16)).astype(jnp.int32)
    slot = jnp.where(named, ranking[:, None, :] + jnp.arange(n_ep) * capacity, 0)
    destination = jnp.sum(slot, axis=2)
    places = jnp.arange(n_ep * capacity, dtype=jnp.int32)
    hit = destination[:, :, None] == places
    pick = jnp.any(hit, axis=1).astype(BF16)
    share = jnp.sum(jnp.where(hit, chosen_expert_weight[:, :, None], 0.0), axis=1)
    share_hi = share.astype(BF16)
    share_lo = (share - share_hi.astype(F32)).astype(BF16)
    send = dot(pick, normed, 0, 0).astype(BF16)
    return fused(
        n_ep,
        query,
        forget_gate_logits,
        value,
        forget_lower_margin,
        jnp.transpose(position_log_decay),
        head_norm_gain[None, :],
        mixer_output_weight,
        send,
        share_hi,
        share_lo,
        gate_weight[0],
        up_weight[0],
        down_weight[0],
    )


def solution(mesh):
    return jax.shard_map(
        body,
        mesh=mesh,
        in_specs=(
            P(("grp", "ep"), "tp"),
            P(("grp", "ep"), "tp"),
            P(("grp", "ep"), "tp"),
            P(None, "tp"),
            P("tp", ("grp", "ep")),
            P(),
            P("tp", None),
            P(("grp", "ep", "tp"), None),
            P(),
            P(("grp", "ep", "tp"), None),
            P(("grp", "ep", "tp"), None),
            P("ep", None, "tp"),
            P("ep", None, "tp"),
            P("ep", "tp", None),
        ),
        out_specs=(P(("grp", "ep", "tp"), None), P(("grp", "ep", "tp"), None)),
        check_vma=False,
    )
```
